32 devices in a mesh: sp: 8 (over z, x), tp: 4 (over y, core).
Axes of the slice: x: 2, y: 2, z: 4, core: 2. Of those that a mesh axis runs over, the one named last changes fastest.
Arguments:
- sequence_embeddings: bfloat16 [3072, 2048], P('sp'), may hold values from -6 to 6
- entry_rescale_vector: bfloat16 [2048], replicated, may hold values from 0.099609375 to 1.8984375
- probe_matrix: bfloat16 [2048, 1024], P('sp', 'tp'), may hold values from -0.125 to 0.125
- onward_retain_matrix: bfloat16 [2048, 1024], P('sp', 'tp'), may hold values from -0.125 to 0.125
- reverse_retain_matrix: bfloat16 [2048, 1024], P('sp', 'tp'), may hold values from -0.125 to 0.125
- content_matrix: bfloat16 [2048, 1024], P('sp', 'tp'), may hold values from -0.125 to 0.125
- emission_switch_matrix: bfloat16 [2048, 1024], P('sp', 'tp'), may hold values from -0.125 to 0.125
- pointwise_content_matrix: bfloat16 [2048, 1024], P('sp', 'tp'), may hold values from -0.125 to 0.125
- pointwise_switch_matrix: bfloat16 [2048, 1024], P('sp', 'tp'), may hold values from -0.125 to 0.125
- retain_lower_slack: float32 [2, 1024], P(None, 'tp'), may hold values from 0 to 0.034, as said below
- extra_log_shrink: float32 [2, 3072, 8], P(None, 'sp', 'tp'), may hold values from -1 to 0
- subspace_rescale: bfloat16 [128], replicated, may hold values from 0.099609375 to 1.8984375
- filter_kernel_coefs: bfloat16 [31, 1024], P(None, 'tp'), may hold values from -1 to 1
- channel_cluster_scale: bfloat16 [1024], P('tp'), may hold values from 0.099609375 to 1.8984375
- scan_readout_matrix: bfloat16 [1024, 2048], P('tp', 'sp'), may hold values from -0.125 to 0.125
- filter_readout_matrix: bfloat16 [1024, 2048], P('tp', 'sp'), may hold values from -0.125 to 0.125
Outputs:
- mixed: bfloat16 [3072, 2048], P(('sp', 'tp'))
The draws below stay inside these ranges and needn't reach their ends.
Inputs may be any that keep to these rules, and one draw needn't show every extreme that they name: `retain_lower_slack`: every entry is positive.
All inputs are finite; a program needn't handle non-finite values.
Results may differ from the reference program's by a relative error of at most 0.015.
Values may be sent and summed in bfloat16 or wider, within the bound.
A program may use at most 64 MiB of HBM per device.

```python
import math
import jax
import jax.numpy as jnp
from jax import lax

SCAN_SUBSPACES = 8
KEY_DIM = 128
VALUE_DIM = 128
GROUP_CH = 128
CONV_KW = 31
BLOCK = 64
TOK_DEV = 384
KEY_WIDTH = 1024
REC_WIDTH = 1024
CONV_CH = 1024
D = 2048
TOKENS = 3072


def draw_retain_lower_slack(key, part):
    slow_count = SCAN_SUBSPACES // 2
    order_key = jax.random.fold_in(key, 11)
    fast_key = jax.random.fold_in(key, 12)
    slow_key = jax.random.fold_in(key, 13)
    head_ranks = jnp.stack([jax.random.permutation(jax.random.fold_in(order_key, 1), SCAN_SUBSPACES), jax.random.permutation(jax.random.fold_in(order_key, 2), SCAN_SUBSPACES)])
    is_slow = (head_ranks < slow_count)[:, :, None]
    fast_rate = jnp.exp(jax.random.uniform(fast_key, (2, SCAN_SUBSPACES, KEY_DIM), jnp.float32, math.log(0.01), math.log(0.033)))
    slow_rate = jnp.exp(jax.random.uniform(slow_key, (2, SCAN_SUBSPACES, KEY_DIM), jnp.float32, math.log(0.1), math.log(0.5))) / TOKENS
    return jnp.where(is_slow, slow_rate, fast_rate).reshape(2, SCAN_SUBSPACES * KEY_DIM).astype(jnp.float32)


def draw_extra_log_shrink(key, part):
    level_key = jax.random.fold_in(key, 21)
    place_key = jax.random.fold_in(key, 22)
    depth_key = jax.random.fold_in(key, 23)
    device_levels = jnp.exp(jax.random.uniform(level_key, (2, TOKENS // TOK_DEV, SCAN_SUBSPACES), jnp.float32, math.log(0.1), math.log(0.4))) / TOKENS
    constant_level = -jnp.repeat(device_levels, TOK_DEV, axis=1)
    places = jnp.stack([jnp.stack([jax.random.permutation(jax.random.fold_in(place_key, direction * SCAN_SUBSPACES + head), TOKENS)[:3] for head in range(SCAN_SUBSPACES)], axis=1) for direction in range(2)])
    network_levels = jnp.log(jax.random.uniform(depth_key, (2, 3, SCAN_SUBSPACES), jnp.float32, 0.55, 0.8))
    positions = jnp.arange(TOKENS)[None, :, None, None]
    agreement_tally = positions == places[:, None, :, :]
    extra_log_draws = jnp.sum(jnp.where(agreement_tally, network_levels[:, None, :, :], 0.0), axis=2)
    return (constant_level + extra_log_draws).astype(jnp.float32)


def block_scale(rng, shape, shards, smallest, high):
    loudness = 1.0
    for position, parts in shards:
        steps = jax.random.uniform(jax.random.fold_in(jax.random.fold_in(rng, 6), position), (parts,), jnp.float32, smallest / len(shards), high / len(shards))
        loudness = loudness * jnp.repeat(jnp.exp(steps), shape[position] // parts).reshape((-1,) + (1,) * (len(shape) - 1 - position))
    return loudness


def normal_values(rng, dims, width, bound, pieces=(), held_as=jnp.bfloat16):
    array = jax.random.normal(rng, dims, jnp.float32) * width
    if len(pieces) > 0:
        array = block_scale(rng, dims, pieces, -0.22, 0.18) * array
    return jnp.clip(array, min=-bound, max=bound).astype(held_as)


def setup_inputs(seed: int = 0) -> dict:
    streams_of = jax.random.split(jax.random.key(seed), 17)
    return {
        "sequence_embeddings": normal_values(streams_of[0], (TOKENS, D), 1.0, 6.0, ((0, 8),)),
        "entry_rescale_vector": jnp.clip(1.0 + 0.18 * jax.random.normal(streams_of[1], (D,), jnp.float32), 0.099609375, 1.8984375).astype(jnp.bfloat16),
        "probe_matrix": normal_values(streams_of[2], (D, KEY_WIDTH), D ** -0.5, 0.125, ((0, 8), (1, 4))),
        "onward_retain_matrix": normal_values(streams_of[3], (D, KEY_WIDTH), D ** -0.5, 0.125, ((0, 8), (1, 4))),
        "reverse_retain_matrix": normal_values(streams_of[4], (D, KEY_WIDTH), D ** -0.5, 0.125, ((0, 8), (1, 4))),
        "content_matrix": normal_values(streams_of[5], (D, REC_WIDTH), D ** -0.5, 0.125, ((0, 8), (1, 4))),
        "emission_switch_matrix": normal_values(streams_of[6], (D, REC_WIDTH), D ** -0.5, 0.125, ((0, 8), (1, 4))),
        "pointwise_content_matrix": normal_values(streams_of[7], (D, CONV_CH), D ** -0.5, 0.125, ((0, 8), (1, 4))),
        "pointwise_switch_matrix": normal_values(streams_of[8], (D, CONV_CH), D ** -0.5, 0.125, ((0, 8), (1, 4))),
        "retain_lower_slack": draw_retain_lower_slack(jax.random.fold_in(streams_of[16], 71), 0),
        "extra_log_shrink": draw_extra_log_shrink(jax.random.fold_in(streams_of[16], 71), 0),
        "subspace_rescale": jnp.clip(1.0 + 0.18 * jax.random.normal(streams_of[11], (VALUE_DIM,), jnp.float32), 0.099609375, 1.8984375).astype(jnp.bfloat16),
        "filter_kernel_coefs": normal_values(streams_of[12], (CONV_KW, CONV_CH), CONV_KW ** -0.5, 1.0, ((1, 4),)),
        "channel_cluster_scale": jnp.clip(1.0 + 0.18 * jax.random.normal(streams_of[13], (CONV_CH,), jnp.float32), 0.099609375, 1.8984375).astype(jnp.bfloat16),
        "scan_readout_matrix": normal_values(streams_of[14], (REC_WIDTH, D), D ** -0.5, 0.125, ((0, 4), (1, 8))),
        "filter_readout_matrix": normal_values(streams_of[15], (CONV_CH, D), D ** -0.5, 0.125, ((0, 4), (1, 8))),
    }


precise_setting = lax.Precision.HIGHEST

def normalize(sequence_embeddings, entry_rescale_vector):
    floats = sequence_embeddings.astype(jnp.float32)
    factor = lax.rsqrt(lax.optimization_barrier(jnp.mean(floats * floats, axis=-1, keepdims=True)) + 1e-06)
    return (floats * factor * entry_rescale_vector.astype(jnp.float32)).astype(jnp.bfloat16)

def sigmoid_switch_entries(emission_switch_scores, retain_lower_slack_line, drawn_extra_lines, subspace_amount):
    length = emission_switch_scores.shape[0]
    retain_slack_amount = retain_lower_slack_line.astype(jnp.float32)[None, :] * jax.nn.sigmoid(-emission_switch_scores)
    retain_slack_amount = retain_slack_amount.reshape(length, subspace_amount, -1)
    log_shrink_amount = jnp.log1p(-retain_slack_amount) + drawn_extra_lines.astype(jnp.float32)[:, :, None]
    return (log_shrink_amount, retain_slack_amount)

def block_recurrence(queries, log_shrink_amount, retain_slack_amount, value_rows, initial):
    length, subspace_amount, key_dim = queries.shape
    block_count = length // BLOCK

    def to_blocks(tensor):
        return tensor.reshape(block_count, BLOCK, subspace_amount, tensor.shape[-1])
    lower_mask = jnp.tril(jnp.ones((BLOCK, BLOCK), jnp.float32))

    def advance(state_carried_over, blocked):
        query_block, decay_block, gap_block, value_block_rows = blocked
        running_state = jnp.cumsum(decay_block, axis=0)
        block_grand_total = running_state[-1]
        lifted_values = query_block * jnp.exp(running_state)
        lowered = gap_block * jnp.exp(-running_state)
        scores = jnp.einsum('thk,shk->hts', lifted_values, lowered, precision=precise_setting) * lower_mask
        within_block = jnp.einsum('hts,shv->thv', scores, value_block_rows, precision=precise_setting)
        output_rows = within_block + jnp.einsum('ipm,pmo->ipo', lifted_values, state_carried_over, precision=precise_setting)
        fading_factor = gap_block * jnp.exp(block_grand_total - running_state)
        updated_state = jnp.exp(block_grand_total)[:, :, None] * state_carried_over + jnp.einsum('fwd,fwt->wdt', fading_factor, value_block_rows, precision=precise_setting)
        return (updated_state, output_rows)
    last_state, output_rows = lax.scan(advance, initial, (to_blocks(queries), to_blocks(log_shrink_amount), to_blocks(retain_slack_amount), to_blocks(value_rows)))
    return (output_rows.reshape(length, subspace_amount, value_rows.shape[-1]), last_state)

def readout(summed, subspace_rescale, out_gate):
    length = summed.shape[0]
    factor = lax.rsqrt(lax.optimization_barrier(jnp.mean(summed * summed, axis=-1, keepdims=True)) + 1e-06)
    scaled = summed * factor * subspace_rescale.astype(jnp.float32)
    return (scaled.reshape(length, -1) * jax.nn.silu(out_gate)).astype(jnp.bfloat16)

def depthwise(framed, filter_kernel_coefs):
    channels = framed.shape[1]
    result = lax.conv_general_dilated(framed[None], filter_kernel_coefs[:, None, :], (1,), 'VALID', dimension_numbers=('NWC', 'WIO', 'NWC'), feature_group_count=channels, preferred_element_type=jnp.float32)
    return result[0]

def group_norm_silu(conv_sum, channel_cluster_scale):
    length, channels = conv_sum.shape
    grouped = conv_sum.reshape(length, -1, GROUP_CH)
    centred = grouped - lax.optimization_barrier(jnp.mean(grouped, axis=-1, keepdims=True))
    variance = lax.optimization_barrier(jnp.mean(centred * centred, axis=-1, keepdims=True))
    standard = (centred * lax.rsqrt(variance + 1e-05)).reshape(length, channels)
    return jax.nn.silu(standard * channel_cluster_scale.astype(jnp.float32)).astype(jnp.bfloat16)

def reference(sequence_embeddings, entry_rescale_vector, probe_matrix, onward_retain_matrix, reverse_retain_matrix, content_matrix, emission_switch_matrix, pointwise_content_matrix, pointwise_switch_matrix, retain_lower_slack, extra_log_shrink, subspace_rescale, filter_kernel_coefs, channel_cluster_scale, scan_readout_matrix, filter_readout_matrix):
    normed = normalize(sequence_embeddings, entry_rescale_vector)

    def multiply_by_matrix(matrix):
        return jnp.dot(normed, matrix, preferred_element_type=jnp.float32)
    length = sequence_embeddings.shape[0]
    queries = jax.nn.silu(multiply_by_matrix(probe_matrix)).reshape(length, SCAN_SUBSPACES, KEY_DIM)
    value_rows = multiply_by_matrix(content_matrix).reshape(length, SCAN_SUBSPACES, VALUE_DIM)
    onward_shrink_multiplier, onward_retain_slack = sigmoid_switch_entries(multiply_by_matrix(onward_retain_matrix), retain_lower_slack[0], extra_log_shrink[0], SCAN_SUBSPACES)
    reverse_shrink_multiplier, reverse_retain_slack = sigmoid_switch_entries(multiply_by_matrix(reverse_retain_matrix), retain_lower_slack[1], extra_log_shrink[1], SCAN_SUBSPACES)
    zero_state = jnp.zeros((SCAN_SUBSPACES, KEY_DIM, VALUE_DIM), jnp.float32)
    forward_out = block_recurrence(queries, onward_shrink_multiplier, onward_retain_slack, value_rows, zero_state)[0]
    backward_out = block_recurrence(jnp.flip(queries, 0), jnp.flip(reverse_shrink_multiplier, 0), jnp.flip(reverse_retain_slack, 0), jnp.flip(value_rows, 0), zero_state)[0]
    backward_out = jnp.flip(backward_out, 0)
    rec_out = readout(forward_out + backward_out, subspace_rescale, multiply_by_matrix(emission_switch_matrix))
    glu = (multiply_by_matrix(pointwise_content_matrix) * jax.nn.sigmoid(multiply_by_matrix(pointwise_switch_matrix))).astype(jnp.bfloat16)
    reach = CONV_KW // 2
    framed = jnp.pad(glu, ((reach, reach), (0, 0)))
    conv_out = group_norm_silu(depthwise(framed, filter_kernel_coefs), channel_cluster_scale)
    mixed = jnp.dot(rec_out, scan_readout_matrix, preferred_element_type=jnp.float32) + jnp.dot(conv_out, filter_readout_matrix, preferred_element_type=jnp.float32)
    return mixed.astype(jnp.bfloat16)
```

```python
import functools

import jax
import jax.numpy as jnp
from jax import lax
from jax.experimental import pallas as pl
from jax.experimental.pallas import tpu as pltpu
from jax.sharding import PartitionSpec as P

HEAD = 128
BLK = 128
MESH = pl.DeviceIdType.MESH
F32 = jnp.float32
BF16 = jnp.bfloat16
EDGE = 16


def dot(a, b, dims=((1,), (0,)), precision=None):
    return lax.dot_general(
        a, b, (dims, ((), ())), preferred_element_type=F32, precision=precision
    )


def kernel(
    ns, nt, nx, taps_n,
    x_ref, gain_ref, w_ref, slack_ref, extra_ref, sub_ref, taps_ref, cscale_ref, wo_ref,
    out_ref,
    win, wout, xs, acc, edge_out, edge_in, frame, lifted, local, decay, pack, st, osum, rec, conv,
    part, rbuf,
    in_send, in_recv, out_send, out_recv, halo_send, halo_recv, st_send, st_recv, rs_send, rs_recv,
):
    nz = ns // nx
    s = lax.axis_index("sp")
    t = lax.axis_index("tp")
    z = s // nx
    x = s % nx
    tl, d_model = x_ref.shape
    n_in, kc, ch = w_ref.shape
    nh = ch // HEAD
    nb = tl // BLK
    rows = tl // nt
    nc = wo_ref.shape[2]
    right = z * nx + lax.rem(x + 1, nx)

    barrier = pltpu.get_barrier_semaphore()

    @pl.loop(1, ns)
    def _(k):
        pl.semaphore_signal(
            barrier, inc=1, device_id=(lax.rem(s + k, ns), t), device_id_type=MESH
        )

    @pl.loop(1, nt)
    def _(k):
        pl.semaphore_signal(
            barrier, inc=1, device_id=(s, lax.rem(t + k, nt)), device_id_type=MESH
        )

    pl.semaphore_wait(barrier, ns - 1 + nt - 1)

    def remote(src, buf, b, sends, recvs, direction, to):
        return pltpu.make_async_remote_copy(
            src_ref=src, dst_ref=buf.at[b], send_sem=sends.at[direction, b],
            recv_sem=recvs.at[b], device_id=(to, t), device_id_type=MESH,
        )

    streams = ((w_ref, win, in_send, in_recv), (wo_ref, wout, out_send, out_recv))

    def up(i, b, src):
        own, buf, sends, recvs = streams[i]

        @pl.when(z + 1 < nz)
        def _():
            remote(src, buf, b, sends, recvs, 0, jnp.minimum(s + nx, ns - 1)).start()

    def down(i, b, src):
        own, buf, sends, recvs = streams[i]

        @pl.when(z > 0)
        def _():
            remote(src, buf, b, sends, recvs, 1, jnp.maximum(s - nx, 0)).start()

    def across(i, b, src):
        own, buf, sends, recvs = streams[i]
        if nx > 1:
            remote(src, buf, b, sends, recvs, 2, right).start()

    def arrive(i, b):
        own, buf, sends, recvs = streams[i]
        remote(buf.at[b], buf, b, sends, recvs, 0, right).wait_recv()

    def send_own(i):
        own = streams[i][0]
        up(i, s, own)
        down(i, s, own)
        across(i, s, own)

    def z_stage(i, d, use):
        buf = streams[i][1]

        @pl.when(z - d >= 0)
        def _():
            b = s - d * nx
            arrive(i, b)
            up(i, b, buf.at[b])
            across(i, b, buf.at[b])

        @pl.when(z + d < nz)
        def _():
            b = s + d * nx
            arrive(i, b)
            down(i, b, buf.at[b])
            across(i, b, buf.at[b])

        if use is not None:

            @pl.when(z - d >= 0)
            def _():
                use(s - d * nx)

            @pl.when(z + d < nz)
            def _():
                use(s + d * nx)

    def x_stage(i, d, use):
        buf = streams[i][1]
        for e in range(1, nx):
            column = lax.rem(x + nx - e, nx)

            def one(zz):
                b = zz * nx + column
                arrive(i, b)
                if e < nx - 1:
                    across(i, b, buf.at[b])
                if use is not None:
                    use(b)

            @pl.when(z - d >= 0)
            def _():
                one(z - d)

            if d > 0:

                @pl.when(z + d < nz)
                def _():
                    one(z + d)

    def finish(i):
        own, buf, sends, recvs = streams[i]
        for zz in range(nz):
            b = zz * nx + x

            @pl.when((z + 1 < nz) & (zz <= z))
            def _():
                remote(own, buf, b, sends, recvs, 0, right).wait_send()

            @pl.when((z > 0) & (zz >= z))
            def _():
                remote(own, buf, b, sends, recvs, 1, right).wait_send()

            for e in range(nx - 1):
                c = zz * nx + lax.rem(x + nx - e, nx)
                remote(own, buf, c, sends, recvs, 2, right).wait_send()

    send_own(0)

    floats = x_ref[...].astype(F32)
    factor = lax.rsqrt(jnp.mean(floats * floats, axis=-1, keepdims=True) + 1e-06)
    for b in range(ns):
        cols = slice(b * kc, (b + 1) * kc)
        xs[b] = (
            x_ref[:, cols].astype(F32) * factor * gain_ref[:, cols].astype(F32)
        ).astype(BF16)

    @pl.loop(0, n_in)
    def _(m):
        acc[m] = dot(xs[s], w_ref[m])

    def consume(b):
        @pl.loop(0, n_in)
        def _(m):
            acc[m] += dot(xs[b], win[b, m])

    for d in range(nz + 1):
        if 1 <= d < nz:
            z_stage(0, d, consume)
        if d == nz - 1:
            send_own(1)
        if d >= 1:
            x_stage(0, d - 1, consume)

    glu = acc[5] * jax.nn.sigmoid(acc[6])
    glu = glu.astype(BF16)
    edge_out[0] = glu[:EDGE]
    edge_out[1] = glu[tl - EDGE:]
    frame[EDGE:EDGE + tl] = glu.astype(F32)

    row_i = lax.broadcasted_iota(jnp.int32, (BLK, BLK), 0)
    col_i = lax.broadcasted_iota(jnp.int32, (BLK, BLK), 1)
    first_half = lax.broadcasted_iota(jnp.int32, (16, HEAD), 0) < 8

    for d in range(2):
        keep = (row_i >= col_i) if d == 0 else (row_i <= col_i)
        tri = keep.astype(F32)
        for h in range(nh):
            lanes = slice(h * HEAD, (h + 1) * HEAD)
            state = jnp.zeros((HEAD, HEAD), F32)
            before = jnp.zeros((1, HEAD), F32)
            order = range(nb) if d == 0 else range(nb - 1, -1, -1)
            for n in order:
                rs = slice(n * BLK, (n + 1) * BLK)
                gap = slack_ref[d:d + 1, lanes] * jax.nn.sigmoid(-acc[1 + d, rs, lanes])
                log_decay = jnp.log1p(-gap) + extra_ref[d, rs, h:h + 1]
                cum = dot(tri, log_decay, precision=lax.Precision.HIGHEST)
                mid = cum[BLK // 2:BLK // 2 + 1]
                total = cum[BLK - 1:] if d == 0 else cum[:1]
                centred = cum - mid
                q = acc[0, rs, lanes]
                q = q * jax.nn.sigmoid(q)
                raised = (q * jnp.exp(centred)).astype(BF16)
                lowered = (gap * jnp.exp(-centred)).astype(BF16)
                v = acc[3, rs, lanes].astype(BF16)
                scores = jnp.where(keep, dot(raised, lowered, ((1,), (1,))), 0.0)
                inside = dot(scores.astype(BF16), v)
                if d == 0:
                    osum[rs, lanes] = inside
                else:
                    osum[rs, lanes] += inside
                lifted[d, h, rs] = raised
                local[d, h, n] = state * jnp.exp(mid)
                decay[d, h, n] = jnp.broadcast_to(before + mid, (8, HEAD))
                added = dot(v, lowered, ((0,), (0,)))
                state = state * jnp.exp(total) + added * jnp.exp(total - mid)
                before = before + total
            pack[d, h, :HEAD] = state.astype(BF16)
            high = before.astype(BF16).astype(F32)
            pack[d, h, HEAD:] = jnp.where(first_half, high, before - high).astype(BF16)

    def state_copy(d, peer, slot):
        return pltpu.make_async_remote_copy(
            src_ref=pack.at[d], dst_ref=st.at[slot], send_sem=st_send.at[peer],
            recv_sem=st_recv.at[slot], device_id=(peer, t), device_id_type=MESH,
        )

    def halo_copy(side, peer):
        return pltpu.make_async_remote_copy(
            src_ref=edge_out.at[side], dst_ref=edge_in.at[1 - side], send_sem=halo_send.at[side],
            recv_sem=halo_recv.at[1 - side], device_id=(peer, t), device_id_type=MESH,
        )

    @pl.when(s > 0)
    def _():
        halo_copy(0, jnp.maximum(s - 1, 0)).start()

    @pl.when(s < ns - 1)
    def _():
        halo_copy(1, jnp.minimum(s + 1, ns - 1)).start()

    @pl.loop(s + 1, ns)
    def _(p):
        state_copy(0, p, s).start()

    @pl.loop(0, s)
    def _(p):
        state_copy(1, p, s).start()

    for d in range(1, nz):
        z_stage(1, d, None)

    @pl.when(s > 0)
    def _():
        halo_copy(1, 0).wait_recv()
        frame[:EDGE] = edge_in[0].astype(F32)

    @pl.when(s == 0)
    def _():
        frame[:EDGE] = jnp.zeros((EDGE, ch), F32)

    @pl.when(s < ns - 1)
    def _():
        halo_copy(0, 0).wait_recv()
        frame[EDGE + tl:] = edge_in[1].astype(F32)

    @pl.when(s == ns - 1)
    def _():
        frame[EDGE + tl:] = jnp.zeros((EDGE, ch), F32)

    off = EDGE - taps_n // 2
    step = 64
    for g in range(nh):
        lanes = slice(g * HEAD, (g + 1) * HEAD)
        taps = taps_ref[:, lanes].astype(F32)
        for r in range(0, tl, step):
            total = jnp.zeros((step, HEAD), F32)
            for j in range(taps_n):
                total += taps[j:j + 1] * frame[r + j + off:r + j + off + step, lanes]
            total = total - jnp.mean(total, axis=-1, keepdims=True)
            var = jnp.mean(total * total, axis=-1, keepdims=True)
            y = total * lax.rsqrt(var + 1e-05) * cscale_ref[:, lanes].astype(F32)
            conv[r:r + step, lanes] = (y * jax.nn.sigmoid(y)).astype(BF16)

    for d in range(nz):
        x_stage(1, d, None)

    def join(d, b, state):
        got = st[b].astype(F32)
        shrink = jnp.exp(got[:, HEAD:HEAD + 1] + got[:, HEAD + 8:HEAD + 9])
        return state * shrink + got[:, :HEAD]

    def ahead(b, state):
        state_copy(0, b, b).wait_recv()
        return join(0, b, state)

    def behind(k, state):
        b = ns - 1 - k
        state_copy(1, b, b).wait_recv()
        return join(1, b, state)

    zero = jnp.zeros((nh, HEAD, HEAD), F32)
    incoming = (lax.fori_loop(0, s, ahead, zero), lax.fori_loop(0, ns - 1 - s, behind, zero))

    for h in range(nh):
        lanes = slice(h * HEAD, (h + 1) * HEAD)
        for n in range(nb):
            rs = slice(n * BLK, (n + 1) * BLK)
            o = osum[rs, lanes]
            for d in range(2):
                full = local[d, h, n] + incoming[d][h] * jnp.exp(decay[d, h, n, :1])
                o += dot(lifted[d, h, rs], full.astype(BF16), ((1,), (1,)))
            norm = lax.rsqrt(jnp.mean(o * o, axis=-1, keepdims=True) + 1e-06)
            e = acc[4, rs, lanes]
            rec[rs, lanes] = (
                o * norm * sub_ref[...].astype(F32) * (e * jax.nn.sigmoid(e))
            ).astype(BF16)

    wout[s] = wo_ref[...]
    for b in range(ns):
        cols = slice(b * nc, (b + 1) * nc)
        y = dot(rec[...], wout[b, 0]) + dot(conv[...], wout[b, 1])
        y = y.astype(BF16)
        for k in range(nt):
            part[k, :, cols] = y[k * rows:(k + 1) * rows]

    def sum_copy(peer, slot):
        return pltpu.make_async_remote_copy(
            src_ref=part.at[peer], dst_ref=rbuf.at[slot], send_sem=rs_send.at[peer],
            recv_sem=rs_recv.at[slot], device_id=(s, peer), device_id_type=MESH,
        )

    for k in range(1, nt):
        sum_copy(lax.rem(t + k, nt), t).start()

    finish(0)
    finish(1)

    @pl.when(s > 0)
    def _():
        halo_copy(0, 0).wait_send()

    @pl.when(s < ns - 1)
    def _():
        halo_copy(1, 0).wait_send()

    @pl.loop(s + 1, ns)
    def _(p):
        state_copy(0, p, s).wait_send()

    @pl.loop(0, s)
    def _(p):
        state_copy(1, p, s).wait_send()

    for k in range(1, nt):
        peer = lax.rem(t + k, nt)
        sum_copy(peer, peer).wait_recv()

    total = part[t].astype(F32)
    for k in range(1, nt):
        total += rbuf[lax.rem(t + k, nt)].astype(F32)
    out_ref[...] = total.astype(BF16)
    for k in range(1, nt):
        peer = lax.rem(t + k, nt)
        sum_copy(peer, peer).wait_send()


def on_device(ns, nt, nx, x, gain, w0, w1, w2, w3, w4, w5, w6, slack, extra, sub, taps, cscale, wa, wb):
    weights = jnp.stack((w0, w1, w2, w3, w4, w5, w6))
    readout = jnp.stack((wa, wb))
    tl, d_model = x.shape
    n_in, kc, ch = weights.shape
    nh = ch // HEAD
    nb = tl // BLK
    nc = readout.shape[2]
    rows = tl // nt
    dma = pltpu.SemaphoreType.DMA
    vmem = pl.BlockSpec(memory_space=pltpu.VMEM)
    return pl.pallas_call(
        functools.partial(kernel, ns, nt, nx, taps.shape[0]),
        out_shape=jax.ShapeDtypeStruct((rows, d_model), BF16),
        in_specs=[vmem] * 9,
        out_specs=vmem,
        scratch_shapes=[
            pltpu.VMEM((ns, n_in, kc, ch), BF16),
            pltpu.VMEM((ns, 2, ch, nc), BF16),
            pltpu.VMEM((ns, tl, kc), BF16),
            pltpu.VMEM((n_in, tl, ch), F32),
            pltpu.VMEM((2, EDGE, ch), BF16),
            pltpu.VMEM((2, EDGE, ch), BF16),
            pltpu.VMEM((tl + 2 * EDGE, ch), F32),
            pltpu.VMEM((2, nh, tl, HEAD), BF16),
            pltpu.VMEM((2, nh, nb, HEAD, HEAD), F32),
            pltpu.VMEM((2, nh, nb, 8, HEAD), F32),
            pltpu.VMEM((2, nh, HEAD + 16, HEAD), BF16),
            pltpu.VMEM((ns, nh, HEAD + 16, HEAD), BF16),
            pltpu.VMEM((tl, ch), F32),
            pltpu.VMEM((tl, ch), BF16),
            pltpu.VMEM((tl, ch), BF16),
            pltpu.VMEM((nt, rows, d_model), BF16),
            pltpu.VMEM((nt, rows, d_model), BF16),
            dma((3, ns)), dma((ns,)), dma((3, ns)), dma((ns,)),
            dma((2,)), dma((2,)), dma((ns,)), dma((ns,)), dma((nt,)), dma((nt,)),
        ],
        compiler_params=pltpu.CompilerParams(
            collective_id=0, has_side_effects=True, vmem_limit_bytes=60 * 1024 * 1024
        ),
    )(
        x, gain.reshape(1, -1), weights, slack, extra, sub.reshape(1, -1), taps,
        cscale.reshape(1, -1), readout,
    )


def solution(mesh):
    ns, nt = mesh.shape["sp"], mesh.shape["tp"]
    nx = max(nt // 2, 1)
    return jax.shard_map(
        functools.partial(on_device, ns, nt, nx),
        mesh=mesh,
        in_specs=(
            P("sp", None),
            P(),
            P("sp", "tp"),
            P("sp", "tp"),
            P("sp", "tp"),
            P("sp", "tp"),
            P("sp", "tp"),
            P("sp", "tp"),
            P("sp", "tp"),
            P(None, "tp"),
            P(None, "sp", "tp"),
            P(),
            P(None, "tp"),
            P("tp"),
            P("tp", "sp"),
            P("tp", "sp"),
        ),
        out_specs=P(("sp", "tp"), None),
        check_vma=False,
    )
```

```python
import functools

import jax
import jax.numpy as jnp
from jax import lax
from jax.experimental import pallas as pl
from jax.experimental.pallas import tpu as pltpu
from jax.sharding import PartitionSpec as P

HEAD = 128
BLK = 128
MESH = pl.DeviceIdType.MESH
F32 = jnp.float32
BF16 = jnp.bfloat16
EDGE = 16


def dot(a, b, dims=((1,), (0,)), precision=None):
    return lax.dot_general(
        a, b, (dims, ((), ())), preferred_element_type=F32, precision=precision
    )


def kernel(
    ns, nt, nx, taps_n,
    *refs,
):
    w_refs = refs[:9]
    kernel_body(ns, nt, nx, taps_n, w_refs, *refs[9:])


def kernel_body(
    ns, nt, nx, taps_n, w_refs,
    x_hbm, gain_ref, slack_ref, extra_ref, sub_ref, taps_ref, cscale_ref,
    out_ref,
    x_ref,
    win_a, win_b, wout, xs, acc, edge_out, edge_in, frame, lifted, local, decay, pack, st, osum, rec, conv,
    part, cbuf, final, part2, rbuf,
    a_send, a_recv, b_send, b_recv, out_send, out_recv, halo_send, halo_recv, st_send, st_recv, c_send, c_recv,
    y_send, y_recv, load_sem,
):
    nz = ns // nx
    s = lax.axis_index("sp")
    t = lax.axis_index("tp")
    z = s // nx
    x = s % nx
    tl, d_model = x_ref.shape
    n_a, kc, ch = win_a.shape[1:]
    n_b = win_b.shape[1]
    nh = ch // HEAD
    nb = tl // BLK
    rows = tl // nt
    nc = wout.shape[3]
    right = z * nx + lax.rem(x + 1, nx)

    loads = [
        pltpu.make_async_copy(w_refs[m], buf.at[s, m - base], load_sem.at[m])
        for buf, base, count in ((win_a, 0, n_a), (win_b, n_a, n_b), (wout, n_a + n_b, 2))
        for m in range(base, base + count)
    ]
    loads.append(pltpu.make_async_copy(x_hbm, x_ref, load_sem.at[n_a + n_b + 2]))
    for load in loads:
        load.start()

    barrier = pltpu.get_barrier_semaphore()

    @pl.loop(1, ns)
    def _(k):
        pl.semaphore_signal(
            barrier, inc=1, device_id=(lax.rem(s + k, ns), t), device_id_type=MESH
        )

    @pl.loop(1, nt)
    def _(k):
        pl.semaphore_signal(
            barrier, inc=1, device_id=(s, lax.rem(t + k, nt)), device_id_type=MESH
        )

    pl.semaphore_wait(barrier, ns - 1 + nt - 1)

    def remote(src, buf, b, sends, recvs, direction, to):
        return pltpu.make_async_remote_copy(
            src_ref=src, dst_ref=buf.at[b], send_sem=sends.at[direction, b],
            recv_sem=recvs.at[b], device_id=(to, t), device_id_type=MESH,
        )

    streams = (
        (win_a.at[s], win_a, a_send, a_recv),
        (win_b.at[s], win_b, b_send, b_recv),
        (wout.at[s], wout, out_send, out_recv),
    )

    def up(i, b, src):
        own, buf, sends, recvs = streams[i]

        @pl.when(z + 1 < nz)
        def _():
            remote(src, buf, b, sends, recvs, 0, jnp.minimum(s + nx, ns - 1)).start()

    def down(i, b, src):
        own, buf, sends, recvs = streams[i]

        @pl.when(z > 0)
        def _():
            remote(src, buf, b, sends, recvs, 1, jnp.maximum(s - nx, 0)).start()

    def across(i, b, src):
        own, buf, sends, recvs = streams[i]
        if nx > 1:
            remote(src, buf, b, sends, recvs, 2, right).start()

    def arrive(i, b):
        own, buf, sends, recvs = streams[i]
        remote(buf.at[b], buf, b, sends, recvs, 0, right).wait_recv()

    def send_own(i):
        own = streams[i][0]
        up(i, s, own)
        down(i, s, own)
        across(i, s, own)

    def z_stage(i, d, use):
        buf = streams[i][1]

        @pl.when(z - d >= 0)
        def _():
            b = s - d * nx
            arrive(i, b)
            up(i, b, buf.at[b])
            across(i, b, buf.at[b])

        @pl.when(z + d < nz)
        def _():
            b = s + d * nx
            arrive(i, b)
            down(i, b, buf.at[b])
            across(i, b, buf.at[b])

        if use is not None:

            @pl.when(z - d >= 0)
            def _():
                use(s - d * nx)

            @pl.when(z + d < nz)
            def _():
                use(s + d * nx)

    def wide_first():
        for e in range(1, nx):
            b = z * nx + lax.rem(x + nx - e, nx)
            arrive(2, b)
            if e < nx - 1:
                across(2, b, wout.at[b])
            up(2, b, wout.at[b])
            down(2, b, wout.at[b])

    def wide_stage(d):
        for column in range(nx):

            @pl.when(z - d >= 0)
            def _():
                b = (z - d) * nx + column
                arrive(2, b)
                up(2, b, wout.at[b])

            @pl.when(z + d < nz)
            def _():
                b = (z + d) * nx + column
                arrive(2, b)
                down(2, b, wout.at[b])

    def x_stage(i, d, use):
        buf = streams[i][1]
        for e in range(1, nx):
            column = lax.rem(x + nx - e, nx)

            def one(zz):
                b = zz * nx + column
                arrive(i, b)
                if e < nx - 1:
                    across(i, b, buf.at[b])
                if use is not None:
                    use(b)

            @pl.when(z - d >= 0)
            def _():
                one(z - d)

            if d > 0:

                @pl.when(z + d < nz)
                def _():
                    one(z + d)

    def finish(i):
        own, buf, sends, recvs = streams[i]
        for zz in range(nz):
            b = zz * nx + x

            @pl.when((z + 1 < nz) & (zz <= z))
            def _():
                remote(own, buf, b, sends, recvs, 0, right).wait_send()

            @pl.when((z > 0) & (zz >= z))
            def _():
                remote(own, buf, b, sends, recvs, 1, right).wait_send()

            for e in range(nx - 1):
                c = zz * nx + lax.rem(x + nx - e, nx)
                remote(own, buf, c, sends, recvs, 2, right).wait_send()

    def wide_finish():
        own, buf, sends, recvs = streams[2]
        for zz in range(nz):
            for column in range(nx):
                b = zz * nx + column

                @pl.when((z + 1 < nz) & (zz <= z))
                def _():
                    remote(own, buf, b, sends, recvs, 0, right).wait_send()

                @pl.when((z > 0) & (zz >= z))
                def _():
                    remote(own, buf, b, sends, recvs, 1, right).wait_send()

        for e in range(nx - 1):
            c = z * nx + lax.rem(x + nx - e, nx)
            remote(own, buf, c, sends, recvs, 2, right).wait_send()

    for load in loads[:n_a]:
        load.wait()
    send_own(0)
    for load in loads[n_a:]:
        load.wait()

    floats = x_ref[...].astype(F32)
    factor = lax.rsqrt(jnp.mean(floats * floats, axis=-1, keepdims=True) + 1e-06)
    for b in range(ns):
        cols = slice(b * kc, (b + 1) * kc)
        xs[b] = (
            x_ref[:, cols].astype(F32) * factor * gain_ref[:, cols].astype(F32)
        ).astype(BF16)

    @pl.loop(0, n_a)
    def _(m):
        acc[m] = dot(xs[s], win_a[s, m])

    @pl.loop(0, n_b)
    def _(m):
        acc[n_a + m] = dot(xs[s], win_b[s, m])

    def consume_a(b):
        @pl.loop(0, n_a)
        def _(m):
            acc[m] += dot(xs[b], win_a[b, m])

    def consume_b(b):
        @pl.loop(0, n_b)
        def _(m):
            acc[n_a + m] += dot(xs[b], win_b[b, m])

    for d in range(nz + 1):
        if 1 <= d < nz:
            z_stage(0, d, consume_a)
        if d == nz - 1:
            across(2, s, wout.at[s])
            send_own(1)
        if d >= 1:
            x_stage(0, d - 1, consume_a)

    row_i = lax.broadcasted_iota(jnp.int32, (BLK, BLK), 0)
    col_i = lax.broadcasted_iota(jnp.int32, (BLK, BLK), 1)
    first_half = lax.broadcasted_iota(jnp.int32, (16, HEAD), 0) < 8

    z_done = 1
    for d in range(2):
        keep = (row_i >= col_i) if d == 0 else (row_i <= col_i)
        tri = keep.astype(F32)
        for h in range(nh):
            lanes = slice(h * HEAD, (h + 1) * HEAD)
            state = jnp.zeros((HEAD, HEAD), F32)
            before = jnp.zeros((1, HEAD), F32)
            order = range(nb) if d == 0 else range(nb - 1, -1, -1)
            for n in order:
                rs = slice(n * BLK, (n + 1) * BLK)
                gap = slack_ref[d:d + 1, lanes] * jax.nn.sigmoid(-acc[1 + d, rs, lanes])
                log_decay = jnp.log1p(-gap) + extra_ref[d, rs, h:h + 1]
                cum = dot(tri, log_decay, precision=lax.Precision.HIGHEST)
                mid = cum[BLK // 2:BLK // 2 + 1]
                total = cum[BLK - 1:] if d == 0 else cum[:1]
                centred = cum - mid
                q = acc[0, rs, lanes]
                q = q * jax.nn.sigmoid(q)
                raised = (q * jnp.exp(centred)).astype(BF16)
                lowered = (gap * jnp.exp(-centred)).astype(BF16)
                v = acc[3, rs, lanes].astype(BF16)
                scores = jnp.where(keep, dot(raised, lowered, ((1,), (1,))), 0.0)
                inside = dot(scores.astype(BF16), v)
                if d == 0:
                    osum[rs, lanes] = inside
                else:
                    osum[rs, lanes] += inside
                lifted[d, h, rs] = raised
                local[d, h, n] = state * jnp.exp(mid)
                decay[d, h, n] = jnp.broadcast_to(before + mid, (8, HEAD))
                added = dot(v, lowered, ((0,), (0,)))
                state = state * jnp.exp(total) + added * jnp.exp(total - mid)
                before = before + total
            pack[d, h, :HEAD] = state.astype(BF16)
            high = before.astype(BF16).astype(F32)
            pack[d, h, HEAD:] = jnp.where(first_half, high, before - high).astype(BF16)
            if (d * nh + h) % 2 == 0 and z_done < nz:
                z_stage(1, z_done, consume_b)
                z_done += 1

    def state_copy(d, peer, slot):
        return pltpu.make_async_remote_copy(
            src_ref=pack.at[d], dst_ref=st.at[slot], send_sem=st_send.at[peer],
            recv_sem=st_recv.at[slot], device_id=(peer, t), device_id_type=MESH,
        )

    def halo_copy(side, peer):
        return pltpu.make_async_remote_copy(
            src_ref=edge_out.at[side], dst_ref=edge_in.at[1 - side], send_sem=halo_send.at[side],
            recv_sem=halo_recv.at[1 - side], device_id=(peer, t), device_id_type=MESH,
        )

    @pl.loop(s + 1, ns)
    def _(p):
        state_copy(0, p, s).start()

    @pl.loop(0, s)
    def _(p):
        state_copy(1, p, s).start()

    for d in range(z_done, nz):
        z_stage(1, d, consume_b)
    up(2, s, wout.at[s])
    down(2, s, wout.at[s])
    wide_first()
    for d in range(min(2, nz)):
        x_stage(1, d, consume_b)

    def join(d, b, state):
        got = st[b].astype(F32)
        shrink = jnp.exp(got[:, HEAD:HEAD + 1] + got[:, HEAD + 8:HEAD + 9])
        return state * shrink + got[:, :HEAD]

    def ahead(b, state):
        state_copy(0, b, b).wait_recv()
        return join(0, b, state)

    def behind(k, state):
        b = ns - 1 - k
        state_copy(1, b, b).wait_recv()
        return join(1, b, state)

    zero = jnp.zeros((nh, HEAD, HEAD), F32)
    incoming = (lax.fori_loop(0, s, ahead, zero), lax.fori_loop(0, ns - 1 - s, behind, zero))

    for h in range(nh):
        lanes = slice(h * HEAD, (h + 1) * HEAD)
        for n in range(nb):
            rs = slice(n * BLK, (n + 1) * BLK)
            o = osum[rs, lanes]
            for d in range(2):
                full = local[d, h, n] + incoming[d][h] * jnp.exp(decay[d, h, n, :1])
                o += dot(lifted[d, h, rs], full.astype(BF16), ((1,), (1,)))
            norm = lax.rsqrt(jnp.mean(o * o, axis=-1, keepdims=True) + 1e-06)
            osum[rs, lanes] = o * norm * sub_ref[...].astype(F32)

    for d in range(2, nz):
        wide_stage(d - 1)
        x_stage(1, d, consume_b)

    glu = acc[n_a + 1] * jax.nn.sigmoid(acc[n_a + 2])
    glu = glu.astype(BF16)
    edge_out[0] = glu[:EDGE]
    edge_out[1] = glu[tl - EDGE:]
    frame[EDGE:EDGE + tl] = glu.astype(F32)

    @pl.when(s > 0)
    def _():
        halo_copy(0, jnp.maximum(s - 1, 0)).start()

    @pl.when(s < ns - 1)
    def _():
        halo_copy(1, jnp.minimum(s + 1, ns - 1)).start()

    e = acc[n_a]
    rec[...] = (osum[...] * (e * jax.nn.sigmoid(e))).astype(BF16)

    @pl.when(s > 0)
    def _():
        halo_copy(1, 0).wait_recv()
        frame[:EDGE] = edge_in[0].astype(F32)

    @pl.when(s == 0)
    def _():
        frame[:EDGE] = jnp.zeros((EDGE, ch), F32)

    @pl.when(s < ns - 1)
    def _():
        halo_copy(0, 0).wait_recv()
        frame[EDGE + tl:] = edge_in[1].astype(F32)

    @pl.when(s == ns - 1)
    def _():
        frame[EDGE + tl:] = jnp.zeros((EDGE, ch), F32)

    off = EDGE - taps_n // 2
    step = 64
    for g in range(nh):
        lanes = slice(g * HEAD, (g + 1) * HEAD)
        taps = taps_ref[:, lanes].astype(F32)
        for r in range(0, tl, step):
            total = jnp.zeros((step, HEAD), F32)
            for j in range(taps_n):
                total += taps[j:j + 1] * frame[r + j + off:r + j + off + step, lanes]
            total = total - jnp.mean(total, axis=-1, keepdims=True)
            var = jnp.mean(total * total, axis=-1, keepdims=True)
            y = total * lax.rsqrt(var + 1e-05) * cscale_ref[:, lanes].astype(F32)
            conv[r:r + step, lanes] = (y * jax.nn.sigmoid(y)).astype(BF16)

    if nz > 1:
        wide_stage(nz - 1)

    half = nt // 2
    mine = lax.rem(t, 2)
    place = t // 2
    other = 1 - mine

    def core_copy(b):
        return pltpu.make_async_remote_copy(
            src_ref=part.at[b, other], dst_ref=cbuf.at[b], send_sem=c_send.at[b],
            recv_sem=c_recv.at[b], device_id=(s, 2 * place + other), device_id_type=MESH,
        )

    def y_copy(b, peer, slot):
        return pltpu.make_async_remote_copy(
            src_ref=part2.at[b, peer], dst_ref=rbuf.at[b, slot], send_sem=y_send.at[b, peer],
            recv_sem=y_recv.at[b, slot], device_id=(s, 2 * peer + mine), device_id_type=MESH,
        )

    @pl.loop(0, ns)
    def _(b):
        y = dot(rec[...], wout[b, 0]) + dot(conv[...], wout[b, 1])
        y = y.astype(BF16)
        for k in range(nt):
            part[b, k % 2, k // 2] = y[k * rows:(k + 1) * rows]
        core_copy(b).start()

    @pl.loop(0, ns)
    def _(b):
        core_copy(b).wait_recv()
        for k in range(1, half):
            peer = lax.rem(place + k, half)
            part2[b, peer] = (
                part[b, mine, peer].astype(F32) + cbuf[b, peer].astype(F32)
            ).astype(BF16)
            y_copy(b, peer, place).start()
        final[b] = part[b, mine, place].astype(F32) + cbuf[b, place].astype(F32)

    finish(0)
    finish(1)
    wide_finish()

    @pl.when(s > 0)
    def _():
        halo_copy(0, 0).wait_send()

    @pl.when(s < ns - 1)
    def _():
        halo_copy(1, 0).wait_send()

    @pl.loop(s + 1, ns)
    def _(p):
        state_copy(0, p, s).wait_send()

    @pl.loop(0, s)
    def _(p):
        state_copy(1, p, s).wait_send()

    for b in range(ns):
        total = final[b]
        for k in range(1, half):
            peer = lax.rem(place + k, half)
            y_copy(b, peer, peer).wait_recv()
            total += rbuf[b, peer].astype(F32)
        out_ref[:, b * nc:(b + 1) * nc] = total.astype(BF16)

    @pl.loop(0, ns)
    def _(b):
        core_copy(b).wait_send()
        for k in range(1, half):
            peer = lax.rem(place + k, half)
            y_copy(b, peer, peer).wait_send()


def on_device(ns, nt, nx, x, gain, w0, w1, w2, w3, w4, w5, w6, slack, extra, sub, taps, cscale, wa, wb):
    tl, d_model = x.shape
    n_a, n_b = 4, 3
    kc, ch = w0.shape
    nh = ch // HEAD
    nb = tl // BLK
    nc = wa.shape[1]
    rows = tl // nt
    half = nt // 2
    dma = pltpu.SemaphoreType.DMA
    vmem = pl.BlockSpec(memory_space=pltpu.VMEM)
    return pl.pallas_call(
        functools.partial(kernel, ns, nt, nx, taps.shape[0]),
        out_shape=jax.ShapeDtypeStruct((rows, d_model), BF16),
        in_specs=[pl.BlockSpec(memory_space=pl.ANY)] * 10 + [vmem] * 6,
        out_specs=vmem,
        scratch_shapes=[
            pltpu.VMEM((tl, d_model), BF16),
            pltpu.VMEM((ns, n_a, kc, ch), BF16),
            pltpu.VMEM((ns, n_b, kc, ch), BF16),
            pltpu.VMEM((ns, 2, ch, nc), BF16),
            pltpu.VMEM((ns, tl, kc), BF16),
            pltpu.VMEM((n_a + n_b, tl, ch), F32),
            pltpu.VMEM((2, EDGE, ch), BF16),
            pltpu.VMEM((2, EDGE, ch), BF16),
            pltpu.VMEM((tl + 2 * EDGE, ch), F32),
            pltpu.VMEM((2, nh, tl, HEAD), BF16),
            pltpu.VMEM((2, nh, nb, HEAD, HEAD), F32),
            pltpu.VMEM((2, nh, nb, 8, HEAD), F32),
            pltpu.VMEM((2, nh, HEAD + 16, HEAD), BF16),
            pltpu.VMEM((ns, nh, HEAD + 16, HEAD), BF16),
            pltpu.VMEM((tl, ch), F32),
            pltpu.VMEM((tl, ch), BF16),
            pltpu.VMEM((tl, ch), BF16),
            pltpu.VMEM((ns, 2, half, rows, nc), BF16),
            pltpu.VMEM((ns, half, rows, nc), BF16),
            pltpu.VMEM((ns, rows, nc), F32),
            pltpu.VMEM((ns, half, rows, nc), BF16),
            pltpu.VMEM((ns, half, rows, nc), BF16),
            dma((3, ns)), dma((ns,)), dma((3, ns)), dma((ns,)), dma((3, ns)), dma((ns,)),
            dma((2,)), dma((2,)), dma((ns,)), dma((ns,)), dma((ns,)), dma((ns,)),
            dma((ns, half)), dma((ns, half)), dma((10,)),
        ],
        compiler_params=pltpu.CompilerParams(
            collective_id=0, has_side_effects=True, vmem_limit_bytes=60 * 1024 * 1024
        ),
    )(
        w0, w1, w2, w3, w4, w5, w6, wa, wb, x, gain.reshape(1, -1), slack, extra,
        sub.reshape(1, -1), taps, cscale.reshape(1, -1),
    )


def solution(mesh):
    ns, nt = mesh.shape["sp"], mesh.shape["tp"]
    nx = max(nt // 2, 1)
    return jax.shard_map(
        functools.partial(on_device, ns, nt, nx),
        mesh=mesh,
        in_specs=(
            P("sp", None),
            P(),
            P("sp", "tp"),
            P("sp", "tp"),
            P("sp", "tp"),
            P("sp", "tp"),
            P("sp", "tp"),
            P("sp", "tp"),
            P("sp", "tp"),
            P(None, "tp"),
            P(None, "sp", "tp"),
            P(),
            P(None, "tp"),
            P("tp"),
            P("tp", "sp"),
            P("tp", "sp"),
        ),
        out_specs=P(("sp", "tp"), None),
        check_vma=False,
    )
```

```python
import functools

import jax
import jax.numpy as jnp
from jax import lax
from jax.experimental import pallas as pl
from jax.experimental.pallas import tpu as pltpu
from jax.sharding import PartitionSpec as P

HEAD = 128
BLK = 128
MESH = pl.DeviceIdType.MESH
F32 = jnp.float32
BF16 = jnp.bfloat16
EDGE = 16


def dot(a, b, dims=((1,), (0,)), precision=None):
    return lax.dot_general(
        a, b, (dims, ((), ())), preferred_element_type=F32, precision=precision
    )


def kernel(
    ns, nt, nx, taps_n,
    *refs,
):
    w_refs = refs[:9]
    kernel_body(ns, nt, nx, taps_n, w_refs, *refs[9:])


def kernel_body(
    ns, nt, nx, taps_n, w_refs,
    x_hbm, gain_ref, slack_ref, extra_ref, sub_ref, taps_ref, cscale_ref,
    out_ref,
    x_ref,
    win_a, win_b, wout, xs, acc, edge_out, edge_in, frame, lifted, local, decay, pack, st, osum, rec, conv,
    part, cbuf, final, part2, rbuf,
    a_send, a_recv, b_send, b_recv, out_send, out_recv, halo_send, halo_recv, st_send, st_recv, c_send, c_recv,
    y_send, y_recv, load_sem,
):
    nz = ns // nx
    s = lax.axis_index("sp")
    t = lax.axis_index("tp")
    z = s // nx
    x = s % nx
    tl, d_model = x_ref.shape
    n_a, kc, ch = win_a.shape[1:]
    n_b = win_b.shape[1]
    nh = ch // HEAD
    nb = tl // BLK
    rows = tl // nt
    nc = wout.shape[3]
    right = z * nx + lax.rem(x + 1, nx)

    loads = [
        pltpu.make_async_copy(w_refs[m], buf.at[s, m - base], load_sem.at[m])
        for buf, base, count in ((win_a, 0, n_a), (win_b, n_a, n_b), (wout, n_a + n_b, 2))
        for m in range(base, base + count)
    ]
    loads.append(pltpu.make_async_copy(x_hbm, x_ref, load_sem.at[n_a + n_b + 2]))
    for load in loads:
        load.start()

    barrier = pltpu.get_barrier_semaphore()

    @pl.loop(1, ns)
    def _(k):
        pl.semaphore_signal(
            barrier, inc=1, device_id=(lax.rem(s + k, ns), t), device_id_type=MESH
        )

    @pl.loop(1, nt)
    def _(k):
        pl.semaphore_signal(
            barrier, inc=1, device_id=(s, lax.rem(t + k, nt)), device_id_type=MESH
        )

    pl.semaphore_wait(barrier, ns - 1 + nt - 1)

    def remote(src, buf, b, sends, recvs, direction, to):
        return pltpu.make_async_remote_copy(
            src_ref=src, dst_ref=buf.at[b], send_sem=sends.at[direction, b],
            recv_sem=recvs.at[b], device_id=(to, t), device_id_type=MESH,
        )

    streams = (
        (win_a.at[s], win_a, a_send, a_recv),
        (win_b.at[s], win_b, b_send, b_recv),
        (wout.at[s], wout, out_send, out_recv),
    )

    def up(i, b, src):
        own, buf, sends, recvs = streams[i]

        @pl.when(z + 1 < nz)
        def _():
            remote(src, buf, b, sends, recvs, 0, jnp.minimum(s + nx, ns - 1)).start()

    def down(i, b, src):
        own, buf, sends, recvs = streams[i]

        @pl.when(z > 0)
        def _():
            remote(src, buf, b, sends, recvs, 1, jnp.maximum(s - nx, 0)).start()

    def across(i, b, src):
        own, buf, sends, recvs = streams[i]
        if nx > 1:
            remote(src, buf, b, sends, recvs, 2, right).start()

    def arrive(i, b):
        own, buf, sends, recvs = streams[i]
        remote(buf.at[b], buf, b, sends, recvs, 0, right).wait_recv()

    def send_own(i):
        own = streams[i][0]
        up(i, s, own)
        down(i, s, own)
        across(i, s, own)

    def z_stage(i, d, use):
        buf = streams[i][1]

        @pl.when(z - d >= 0)
        def _():
            b = s - d * nx
            arrive(i, b)
            up(i, b, buf.at[b])
            across(i, b, buf.at[b])

        @pl.when(z + d < nz)
        def _():
            b = s + d * nx
            arrive(i, b)
            down(i, b, buf.at[b])
            across(i, b, buf.at[b])

        if use is not None:

            @pl.when(z - d >= 0)
            def _():
                use(s - d * nx)

            @pl.when(z + d < nz)
            def _():
                use(s + d * nx)

    def wide_first():
        for e in range(1, nx):
            b = z * nx + lax.rem(x + nx - e, nx)
            arrive(2, b)
            if e < nx - 1:
                across(2, b, wout.at[b])
            up(2, b, wout.at[b])
            down(2, b, wout.at[b])

    def wide_stage(d):
        for column in range(nx):

            @pl.when(z - d >= 0)
            def _():
                b = (z - d) * nx + column
                arrive(2, b)
                up(2, b, wout.at[b])

            @pl.when(z + d < nz)
            def _():
                b = (z + d) * nx + column
                arrive(2, b)
                down(2, b, wout.at[b])

    def x_stage(i, d, use):
        buf = streams[i][1]
        for e in range(1, nx):
            column = lax.rem(x + nx - e, nx)

            def one(zz):
                b = zz * nx + column
                arrive(i, b)
                if e < nx - 1:
                    across(i, b, buf.at[b])
                if use is not None:
                    use(b)

            @pl.when(z - d >= 0)
            def _():
                one(z - d)

            if d > 0:

                @pl.when(z + d < nz)
                def _():
                    one(z + d)

    def finish(i):
        own, buf, sends, recvs = streams[i]
        for zz in range(nz):
            b = zz * nx + x

            @pl.when((z + 1 < nz) & (zz <= z))
            def _():
                remote(own, buf, b, sends, recvs, 0, right).wait_send()

            @pl.when((z > 0) & (zz >= z))
            def _():
                remote(own, buf, b, sends, recvs, 1, right).wait_send()

            for e in range(nx - 1):
                c = zz * nx + lax.rem(x + nx - e, nx)
                remote(own, buf, c, sends, recvs, 2, right).wait_send()

    def wide_finish():
        own, buf, sends, recvs = streams[2]
        for zz in range(nz):
            for column in range(nx):
                b = zz * nx + column

                @pl.when((z + 1 < nz) & (zz <= z))
                def _():
                    remote(own, buf, b, sends, recvs, 0, right).wait_send()

                @pl.when((z > 0) & (zz >= z))
                def _():
                    remote(own, buf, b, sends, recvs, 1, right).wait_send()

        for e in range(nx - 1):
            c = z * nx + lax.rem(x + nx - e, nx)
            remote(own, buf, c, sends, recvs, 2, right).wait_send()

    for load in loads[:n_a]:
        load.wait()
    send_own(0)
    for load in loads[n_a:]:
        load.wait()

    floats = x_ref[...].astype(F32)
    factor = lax.rsqrt(jnp.mean(floats * floats, axis=-1, keepdims=True) + 1e-06)
    for b in range(ns):
        cols = slice(b * kc, (b + 1) * kc)
        xs[b] = (
            x_ref[:, cols].astype(F32) * factor * gain_ref[:, cols].astype(F32)
        ).astype(BF16)

    @pl.loop(0, n_a)
    def _(m):
        acc[m] = dot(xs[s], win_a[s, m])

    @pl.loop(0, n_b)
    def _(m):
        acc[n_a + m] = dot(xs[s], win_b[s, m])

    def consume_a(b):
        @pl.loop(0, n_a)
        def _(m):
            acc[m] += dot(xs[b], win_a[b, m])

    def consume_b(b):
        @pl.loop(0, n_b)
        def _(m):
            acc[n_a + m] += dot(xs[b], win_b[b, m])

    for d in range(1, nz):
        z_stage(0, d, consume_a)
    across(2, s, wout.at[s])
    send_own(1)
    for d in range(nz):
        x_stage(0, d, consume_a)

    row_i = lax.broadcasted_iota(jnp.int32, (BLK, BLK), 0)
    col_i = lax.broadcasted_iota(jnp.int32, (BLK, BLK), 1)
    first_half = lax.broadcasted_iota(jnp.int32, (16, HEAD), 0) < 8

    z_done = 1
    for d in range(2):
        keep = (row_i >= col_i) if d == 0 else (row_i <= col_i)
        tri = keep.astype(F32)
        for h in range(nh):
            lanes = slice(h * HEAD, (h + 1) * HEAD)
            state = jnp.zeros((HEAD, HEAD), F32)
            before = jnp.zeros((1, HEAD), F32)
            order = range(nb) if d == 0 else range(nb - 1, -1, -1)
            for n in order:
                rs = slice(n * BLK, (n + 1) * BLK)
                gap = slack_ref[d:d + 1, lanes] * jax.nn.sigmoid(-acc[1 + d, rs, lanes])
                log_decay = jnp.log1p(-gap) + extra_ref[d, rs, h:h + 1]
                cum = dot(tri, log_decay, precision=lax.Precision.HIGHEST)
                mid = cum[BLK // 2:BLK // 2 + 1]
                total = cum[BLK - 1:] if d == 0 else cum[:1]
                centred = cum - mid
                q = acc[0, rs, lanes]
                q = q * jax.nn.sigmoid(q)
                raised = (q * jnp.exp(centred)).astype(BF16)
                lowered = (gap * jnp.exp(-centred)).astype(BF16)
                v = acc[3, rs, lanes].astype(BF16)
                scores = jnp.where(keep, dot(raised, lowered, ((1,), (1,))), 0.0)
                inside = dot(scores.astype(BF16), v)
                if d == 0:
                    osum[rs, lanes] = inside
                else:
                    osum[rs, lanes] += inside
                lifted[d, h, rs] = raised
                local[d, h, n] = state * jnp.exp(mid)
                decay[d, h, n] = jnp.broadcast_to(before + mid, (8, HEAD))
                added = dot(v, lowered, ((0,), (0,)))
                state = state * jnp.exp(total) + added * jnp.exp(total - mid)
                before = before + total
            pack[d, h, :HEAD] = state.astype(BF16)
            high = before.astype(BF16).astype(F32)
            pack[d, h, HEAD:] = jnp.where(first_half, high, before - high).astype(BF16)
            if (d * nh + h) % 2 == 0 and z_done < nz:
                z_stage(1, z_done, consume_b)
                z_done += 1

    def state_copy(d, peer, slot):
        return pltpu.make_async_remote_copy(
            src_ref=pack.at[d], dst_ref=st.at[slot], send_sem=st_send.at[peer],
            recv_sem=st_recv.at[slot], device_id=(peer, t), device_id_type=MESH,
        )

    def halo_copy(side, peer):
        return pltpu.make_async_remote_copy(
            src_ref=edge_out.at[side], dst_ref=edge_in.at[1 - side], send_sem=halo_send.at[side],
            recv_sem=halo_recv.at[1 - side], device_id=(peer, t), device_id_type=MESH,
        )

    @pl.loop(s + 1, ns)
    def _(p):
        state_copy(0, p, s).start()

    @pl.loop(0, s)
    def _(p):
        state_copy(1, p, s).start()

    for d in range(z_done, nz):
        z_stage(1, d, consume_b)
    up(2, s, wout.at[s])
    down(2, s, wout.at[s])
    wide_first()
    x_stage(1, 0, consume_b)
    if nz > 1:
        if nz > 2:
            wide_stage(1)
        x_stage(1, 1, consume_b)

    def join(d, b, state):
        got = st[b].astype(F32)
        shrink = jnp.exp(got[:, HEAD:HEAD + 1] + got[:, HEAD + 8:HEAD + 9])
        return state * shrink + got[:, :HEAD]

    def ahead(b, state):
        state_copy(0, b, b).wait_recv()
        return join(0, b, state)

    def behind(k, state):
        b = ns - 1 - k
        state_copy(1, b, b).wait_recv()
        return join(1, b, state)

    zero = jnp.zeros((nh, HEAD, HEAD), F32)
    incoming = (lax.fori_loop(0, s, ahead, zero), lax.fori_loop(0, ns - 1 - s, behind, zero))

    for h in range(nh):
        lanes = slice(h * HEAD, (h + 1) * HEAD)
        for n in range(nb):
            rs = slice(n * BLK, (n + 1) * BLK)
            o = osum[rs, lanes]
            for d in range(2):
                full = local[d, h, n] + incoming[d][h] * jnp.exp(decay[d, h, n, :1])
                o += dot(lifted[d, h, rs], full.astype(BF16), ((1,), (1,)))
            norm = lax.rsqrt(jnp.mean(o * o, axis=-1, keepdims=True) + 1e-06)
            osum[rs, lanes] = o * norm * sub_ref[...].astype(F32)

    for d in range(2, nz):
        if d > 2:
            wide_stage(d - 1)
        x_stage(1, d, consume_b)

    glu = acc[n_a + 1] * jax.nn.sigmoid(acc[n_a + 2])
    glu = glu.astype(BF16)
    edge_out[0] = glu[:EDGE]
    edge_out[1] = glu[tl - EDGE:]
    frame[EDGE:EDGE + tl] = glu.astype(F32)

    @pl.when(s > 0)
    def _():
        halo_copy(0, jnp.maximum(s - 1, 0)).start()

    @pl.when(s < ns - 1)
    def _():
        halo_copy(1, jnp.minimum(s + 1, ns - 1)).start()

    e = acc[n_a]
    rec[...] = (osum[...] * (e * jax.nn.sigmoid(e))).astype(BF16)

    @pl.when(s > 0)
    def _():
        halo_copy(1, 0).wait_recv()
        frame[:EDGE] = edge_in[0].astype(F32)

    @pl.when(s == 0)
    def _():
        frame[:EDGE] = jnp.zeros((EDGE, ch), F32)

    @pl.when(s < ns - 1)
    def _():
        halo_copy(0, 0).wait_recv()
        frame[EDGE + tl:] = edge_in[1].astype(F32)

    @pl.when(s == ns - 1)
    def _():
        frame[EDGE + tl:] = jnp.zeros((EDGE, ch), F32)

    off = EDGE - taps_n // 2
    step = 64
    for g in range(nh):
        lanes = slice(g * HEAD, (g + 1) * HEAD)
        taps = taps_ref[:, lanes].astype(F32)
        for r in range(0, tl, step):
            total = jnp.zeros((step, HEAD), F32)
            for j in range(taps_n):
                total += taps[j:j + 1] * frame[r + j + off:r + j + off + step, lanes]
            total = total - jnp.mean(total, axis=-1, keepdims=True)
            var = jnp.mean(total * total, axis=-1, keepdims=True)
            y = total * lax.rsqrt(var + 1e-05) * cscale_ref[:, lanes].astype(F32)
            conv[r:r + step, lanes] = (y * jax.nn.sigmoid(y)).astype(BF16)

    if nz > 1:
        wide_stage(nz - 1)

    half = nt // 2
    mine = lax.rem(t, 2)
    place = t // 2
    other = 1 - mine

    def core_copy(b):
        return pltpu.make_async_remote_copy(
            src_ref=part.at[b, other], dst_ref=cbuf.at[b], send_sem=c_send.at[b],
            recv_sem=c_recv.at[b], device_id=(s, 2 * place + other), device_id_type=MESH,
        )

    def y_copy(b, peer, slot):
        return pltpu.make_async_remote_copy(
            src_ref=part2.at[b, peer], dst_ref=rbuf.at[b, slot], send_sem=y_send.at[b, peer],
            recv_sem=y_recv.at[b, slot], device_id=(s, 2 * peer + mine), device_id_type=MESH,
        )

    @pl.loop(0, ns)
    def _(b):
        y = dot(rec[...], wout[b, 0]) + dot(conv[...], wout[b, 1])
        y = y.astype(BF16)
        for k in range(nt):
            part[b, k % 2, k // 2] = y[k * rows:(k + 1) * rows]
        core_copy(b).start()

    @pl.loop(0, ns)
    def _(b):
        core_copy(b).wait_recv()
        for k in range(1, half):
            peer = lax.rem(place + k, half)
            part2[b, peer] = (
                part[b, mine, peer].astype(F32) + cbuf[b, peer].astype(F32)
            ).astype(BF16)
            y_copy(b, peer, place).start()
        final[b] = part[b, mine, place].astype(F32) + cbuf[b, place].astype(F32)

    finish(0)
    finish(1)
    wide_finish()

    @pl.when(s > 0)
    def _():
        halo_copy(0, 0).wait_send()

    @pl.when(s < ns - 1)
    def _():
        halo_copy(1, 0).wait_send()

    @pl.loop(s + 1, ns)
    def _(p):
        state_copy(0, p, s).wait_send()

    @pl.loop(0, s)
    def _(p):
        state_copy(1, p, s).wait_send()

    for b in range(ns):
        total = final[b]
        for k in range(1, half):
            peer = lax.rem(place + k, half)
            y_copy(b, peer, peer).wait_recv()
            total += rbuf[b, peer].astype(F32)
        out_ref[:, b * nc:(b + 1) * nc] = total.astype(BF16)

    @pl.loop(0, ns)
    def _(b):
        core_copy(b).wait_send()
        for k in range(1, half):
            peer = lax.rem(place + k, half)
            y_copy(b, peer, peer).wait_send()


def on_device(ns, nt, nx, x, gain, w0, w1, w2, w3, w4, w5, w6, slack, extra, sub, taps, cscale, wa, wb):
    tl, d_model = x.shape
    n_a, n_b = 4, 3
    kc, ch = w0.shape
    nh = ch // HEAD
    nb = tl // BLK
    nc = wa.shape[1]
    rows = tl // nt
    half = nt // 2
    dma = pltpu.SemaphoreType.DMA
    vmem = pl.BlockSpec(memory_space=pltpu.VMEM)
    return pl.pallas_call(
        functools.partial(kernel, ns, nt, nx, taps.shape[0]),
        out_shape=jax.ShapeDtypeStruct((rows, d_model), BF16),
        in_specs=[pl.BlockSpec(memory_space=pl.ANY)] * 10 + [vmem] * 6,
        out_specs=vmem,
        scratch_shapes=[
            pltpu.VMEM((tl, d_model), BF16),
            pltpu.VMEM((ns, n_a, kc, ch), BF16),
            pltpu.VMEM((ns, n_b, kc, ch), BF16),
            pltpu.VMEM((ns, 2, ch, nc), BF16),
            pltpu.VMEM((ns, tl, kc), BF16),
            pltpu.VMEM((n_a + n_b, tl, ch), F32),
            pltpu.VMEM((2, EDGE, ch), BF16),
            pltpu.VMEM((2, EDGE, ch), BF16),
            pltpu.VMEM((tl + 2 * EDGE, ch), F32),
            pltpu.VMEM((2, nh, tl, HEAD), BF16),
            pltpu.VMEM((2, nh, nb, HEAD, HEAD), F32),
            pltpu.VMEM((2, nh, nb, 8, HEAD), F32),
            pltpu.VMEM((2, nh, HEAD + 16, HEAD), BF16),
            pltpu.VMEM((ns, nh, HEAD + 16, HEAD), BF16),
            pltpu.VMEM((tl, ch), F32),
            pltpu.VMEM((tl, ch), BF16),
            pltpu.VMEM((tl, ch), BF16),
            pltpu.VMEM((ns, 2, half, rows, nc), BF16),
            pltpu.VMEM((ns, half, rows, nc), BF16),
            pltpu.VMEM((ns, rows, nc), F32),
            pltpu.VMEM((ns, half, rows, nc), BF16),
            pltpu.VMEM((ns, half, rows, nc), BF16),
            dma((3, ns)), dma((ns,)), dma((3, ns)), dma((ns,)), dma((3, ns)), dma((ns,)),
            dma((2,)), dma((2,)), dma((ns,)), dma((ns,)), dma((ns,)), dma((ns,)),
            dma((ns, half)), dma((ns, half)), dma((10,)),
        ],
        compiler_params=pltpu.CompilerParams(
            collective_id=0, has_side_effects=True, vmem_limit_bytes=60 * 1024 * 1024
        ),
    )(
        w0, w1, w2, w3, w4, w5, w6, wa, wb, x, gain.reshape(1, -1), slack, extra,
        sub.reshape(1, -1), taps, cscale.reshape(1, -1),
    )


def solution(mesh):
    ns, nt = mesh.shape["sp"], mesh.shape["tp"]
    nx = max(nt // 2, 1)
    return jax.shard_map(
        functools.partial(on_device, ns, nt, nx),
        mesh=mesh,
        in_specs=(
            P("sp", None),
            P(),
            P("sp", "tp"),
            P("sp", "tp"),
            P("sp", "tp"),
            P("sp", "tp"),
            P("sp", "tp"),
            P("sp", "tp"),
            P("sp", "tp"),
            P(None, "tp"),
            P(None, "sp", "tp"),
            P(),
            P(None, "tp"),
            P("tp"),
            P("tp", "sp"),
            P("tp", "sp"),
        ),
        out_specs=P(("sp", "tp"), None),
        check_vma=False,
    )
```
